256 devices in a mesh: grp: 2 (over y), sp: 32 (over z, core), tp: 4 (over x).
Axes of the slice: x: 4, y: 2, z: 16, core: 2. Of those that a mesh axis runs over, the one named last changes fastest.
The devices are a block of a 4x16x16 slice.
Arguments:
- stream: bfloat16 [16384, 4096], P(('grp', 'sp'), 'tp'), parts along dimension 0, may hold values from -6 to 6
- gain_pre: float32 [3, 4096], replicated, may hold values from 0.1 to 1.9
- w_in: bfloat16 [3, 4096, 1024], P(None, 'sp', 'tp'), may hold values from -0.09375 to 0.09375
- w_pool: bfloat16 [3, 4, 256, 256], P(None, 'tp'), may hold values from -0.375 to 0.375
- pool_scale: float32 [3, 1024], P(None, 'tp'), may hold values from 0.1 to 1.9
- w_out: bfloat16 [3, 1024, 4096], P(None, 'tp', 'sp'), may hold values from -0.5 to 0.5
- gain_post: float32 [3, 4096], replicated, may hold values from 0.1 to 1.9
Outputs:
- result: bfloat16 [16384, 4096], P(('grp', 'sp'), 'tp'), parts along dimension 0
The draws below stay inside these ranges and needn't reach their ends.
There are 2 independent parts, one for each index of `grp`. The reference program is written for one: setup_inputs(seed, part) draws one part's arguments, and reference() takes and returns one part's arrays. A program takes and returns all parts, laid end to end along the dimension named above; an argument that names none is the same for every part. Nothing has to cross between parts.
All inputs are finite; a program needn't handle non-finite values.
Results may differ from the reference program's by a relative error of at most 0.02.
Values may be sent and summed in bfloat16 or wider, within the bound.
No kernel may reach another device: no remote copies, remote signals or barrier semaphores. Data moves between devices by JAX's collectives and lax.ppermute only.
A program may use at most 64 MiB of HBM per device.

```python
import jax
import jax.numpy as jnp
from jax import lax

D = 4096
GROUP = 256
POOL = 1024
LAYERS = 3
TOKENS = 8192


def draw_w_out(key, part):
    key_entries = jax.random.fold_in(key, 11)
    key_rough = jax.random.fold_in(key, 12)
    column_place = jnp.arange(D).astype(jnp.float32) / float(D - 1)
    rough = jax.random.uniform(key_rough, (D,), jnp.float32, 0.7, 1.4)
    entries = jax.random.normal(key_entries, (LAYERS, POOL, D), jnp.float32)
    column_scale = 0.4 * jnp.exp(jnp.log(6.0) * column_place) * rough
    values = entries * column_scale[None, None, :] * float(POOL) ** (-0.5)
    values = jnp.clip(values, -0.5, 0.5)
    return values.astype(jnp.bfloat16)


def block_levels(key, shape, pieces, low, high):
    level = 1.0
    for dim, parts in pieces:
        steps = jax.random.uniform(jax.random.fold_in(jax.random.fold_in(key, 6), dim), (parts,), jnp.float32, low / len(pieces), high / len(pieces))
        level = level * jnp.repeat(jnp.exp(steps), shape[dim] // parts).reshape((-1,) + (1,) * (len(shape) - 1 - dim))
    return level


def gaussian(rng, extent, deviation, most, shards=(), dtype=jnp.bfloat16):
    factor_of = block_levels(rng, extent, shards, -0.22, 0.18) if shards else 1.0
    values = jax.random.normal(rng, extent, jnp.float32) * deviation * factor_of
    return jnp.minimum(jnp.maximum(values, -most), most).astype(dtype)


def setup_inputs(seed: int = 0, part: int = 0) -> dict:
    arg_keys = jax.random.split(jax.random.key(seed), 8)
    part_keys = jax.random.split(jax.random.fold_in(arg_keys[7], part), 8)
    return {
        "stream": gaussian(part_keys[0], (TOKENS, D), 1.0, 6.0, ((0, 32), (1, 4))),
        "gain_pre": jnp.clip(1.0 + 0.18 * jax.random.normal(arg_keys[1], (LAYERS, D), jnp.float32), 0.1, 1.9),
        "w_in": gaussian(arg_keys[2], (LAYERS, D, POOL), D ** -0.5, 0.09375, ((1, 32), (2, 4))),
        "w_pool": gaussian(arg_keys[3], (LAYERS, 4, GROUP, GROUP), GROUP ** -0.5, 0.375, ((1, 4),)),
        "pool_scale": jnp.clip(1.0 + 0.18 * jax.random.normal(arg_keys[4], (LAYERS, POOL), jnp.float32), 0.1, 1.9),
        "w_out": draw_w_out(jax.random.fold_in(arg_keys[7], 71), part),
        "gain_post": jnp.clip(1.0 + 0.18 * jax.random.normal(arg_keys[6], (LAYERS, D), jnp.float32), 0.1, 1.9),
    }


WINDOWS = (2, 4, 8, 16)
EPS = 1e-06

def rms_scale(values, gain):
    inverse = lax.rsqrt(lax.optimization_barrier(jnp.mean(values * values, axis=-1, keepdims=True)) + EPS)
    return values * inverse * gain[None, :]

def reference(stream, gain_pre, w_in, w_pool, pool_scale, w_out, gain_post):
    reach = max(WINDOWS) - 1
    positions = jnp.arange(TOKENS).astype(jnp.float32)
    current = stream
    for layer in range(LAYERS):
        normed = rms_scale(current.astype(jnp.float32), gain_pre[layer]).astype(jnp.bfloat16)
        inner = jnp.dot(normed, w_in[layer], preferred_element_type=jnp.float32).astype(jnp.bfloat16)
        inner_f = inner.astype(jnp.float32)
        padded = jnp.concatenate([jnp.zeros((reach, 4 * GROUP), jnp.float32), inner_f], axis=0)
        branch = jnp.zeros((TOKENS, D), jnp.float32)
        for group_id in range(4):
            window = WINDOWS[group_id]
            lo = group_id * GROUP
            summed = jnp.zeros((TOKENS, GROUP), jnp.float32)
            for offset in range(window):
                summed = summed + padded[reach - offset:reach - offset + TOKENS, lo:lo + GROUP]
            count = jnp.minimum(positions + 1.0, float(window))
            pooled = summed / count[:, None]
            spread = (pooled - inner_f[:, lo:lo + GROUP]).astype(jnp.bfloat16)
            mixed = jnp.dot(spread, w_pool[layer, group_id], preferred_element_type=jnp.float32)
            mixed = (mixed * pool_scale[layer, lo:lo + GROUP][None, :]).astype(jnp.bfloat16)
            partial_value = jnp.dot(mixed, w_out[layer, lo:lo + GROUP], preferred_element_type=jnp.float32)
            partial_value = lax.optimization_barrier(partial_value.astype(jnp.bfloat16))
            branch = branch + partial_value.astype(jnp.float32)
        current = (current.astype(jnp.float32) + rms_scale(branch, gain_post[layer])).astype(jnp.bfloat16)
    return current
```

```python
import functools

import jax
import jax.numpy as jnp
from jax import lax
from jax.experimental import pallas as pl
from jax.experimental.pallas import tpu as pltpu
from jax.sharding import PartitionSpec as P

WINDOWS = (2, 4, 8, 16)
EPS = 1e-06
BF16 = jnp.bfloat16
F32 = jnp.float32
HALO_STEP = 16


def call(body, outs, flops=0, nbytes=1 << 20, name=None, **scratch):
    many = isinstance(outs, (list, tuple))
    specs = [pl.BlockSpec(memory_space=pltpu.VMEM) for _ in (outs if many else [outs])]
    return pl.pallas_call(
        body,
        out_shape=outs,
        out_specs=specs if many else specs[0],
        cost_estimate=pl.CostEstimate(flops=flops, bytes_accessed=nbytes, transcendentals=0),
        compiler_params=pltpu.CompilerParams(vmem_limit_bytes=48 << 20),
        name=name,
        **scratch,
    )


def vmem_call(body, outs, *args, **kw):
    fn = functools.partial(call, body, outs, **kw)
    return fn(in_specs=[pl.BlockSpec(memory_space=pltpu.VMEM) for _ in args])(*args)


def shape(s, d):
    return jax.ShapeDtypeStruct(s, d)


def dot(a, b):
    return jnp.dot(a, b, preferred_element_type=F32)


def dot_nt(a, b):
    return lax.dot_general(a, b, (((1,), (1,)), ((), ())), preferred_element_type=F32)


def shifted(array, k):
    n = lax.axis_size("tp")
    return lax.ppermute(array, "tp", [(i, (i + k) % n) for i in range(n)])


def shifts(arrays):
    return [shifted(a, k) for k, a in arrays]


def pairwise(array, stage):
    mate = (lambda i: i ^ 1) if stage == 0 else (lambda i: i ^ 3)
    return lax.ppermute(array, "tp", [(i, mate(i)) for i in range(lax.axis_size("tp"))])


def swapped(array):
    return lax.ppermute(array, "sp", [(s, s ^ 1) for s in range(lax.axis_size("sp"))])


def ring_step(array):
    chips = lax.axis_size("sp") // 2
    down = [(2 * z, 2 * ((z + 1) % chips)) for z in range(chips)]
    up = [(2 * z + 1, 2 * ((z - 1) % chips) + 1) for z in range(chips)]
    return lax.ppermute(array, "sp", down + up)


def transposed_blocks(array):
    n_sp, n_tp = lax.axis_size("sp"), lax.axis_size("tp")
    route = []
    for s in range(n_sp):
        m, a = divmod(s, n_tp)
        for c in range(n_tp):
            route.append((s * n_tp + c, (m * n_tp + c) * n_tp + a))
    return lax.ppermute(array, ("sp", "tp"), route)


def from_behind(block):
    n = lax.axis_size("sp")
    return lax.ppermute(block, "sp", [(i, i + 1) for i in range(n - 1)])


def both_cores(own):
    other = swapped(own)
    first = lax.axis_index("sp") % 2 == 0
    return jnp.where(first, jnp.stack([own, other]), jnp.stack([other, own]))


def assemble_kernel(n_steps, n_mats, *refs):
    chips = 2 * n_steps
    start, rest = refs[0], refs[1:]
    ring, rest = rest[:n_steps], rest[n_steps:]
    half = n_steps // 2
    swaps, outs = rest[:2], rest[2:]
    s = lax.axis_index("sp")
    z = s // 2
    sign = 1 - 2 * (s % 2)

    def put(place, block):
        at = lax.rem(place + 2 * chips, chips)
        for i, out in enumerate(outs):
            out[at] = block[:, i]

    put(z, start[...])
    for k in range(1, n_steps + 1):
        put(z - sign * k, ring[k - 1][...])
    for k in range(1, n_steps):
        ref, i = (swaps[0], k - 1) if k <= half else (swaps[1], k - 1 - half)
        put(z + sign * k, ref[i])


def gathered(own):
    mats, rows, cols = own.shape
    n_steps = lax.axis_size("sp") // 4
    half = n_steps // 2
    start = both_cores(own)
    ring, held = [], start
    for _ in range(n_steps):
        held = ring_step(held)
        ring.append(held)
    near = swapped(jnp.stack(ring[:half]))
    far = swapped(jnp.stack(ring[half : n_steps - 1]))
    outs = [shape((2 * n_steps, 2, rows, cols), BF16)] * mats
    return vmem_call(
        functools.partial(assemble_kernel, n_steps, mats),
        outs,
        start,
        *ring,
        near,
        far,
        nbytes=4 * mats * 4 * n_steps * rows * cols * 2,
        flops=1 << 20,
        name="assemble",
    )


def mix(inner, row0, wp, scale):
    rows = inner.shape[0]
    t = lax.axis_index("tp")
    w = inner
    sums = []
    for k in range(len(WINDOWS)):
        w = w + pltpu.roll(w, 1 << k, 0)
        sums.append(w)
    total = jnp.where(t == 0, sums[0], jnp.where(t == 1, sums[1], jnp.where(t == 2, sums[2], sums[3])))
    window = lax.shift_left(2, t)
    place = row0 + lax.broadcasted_iota(jnp.int32, (rows, 1), 0)
    count = jnp.clip(jnp.minimum(place + 1, window), 1, None).astype(F32)
    spread = (total / count - inner)[HALO_STEP:]
    return (dot(spread.astype(BF16), wp) * scale).astype(BF16)


def head_kernel(halo, x0, x1, x2, x3, gain, w_in, wp, scale, mixed, cur, first_sq):
    t = lax.axis_index("tp")
    n = lax.axis_size("tp")
    rows, width = x0.shape
    chunk = width // (2 * n)
    tok = rows - halo
    acc = None
    squares = None
    for k, x in enumerate((x0, x1, x2, x3)):
        owner = lax.rem(t - k + n, n)
        v = x[...].astype(F32)
        part = jnp.sum(v * v, axis=1, keepdims=True)
        w = w_in[owner]
        scaled = (v * gain[owner]).astype(BF16)
        d = dot(scaled, w)
        acc = d if acc is None else acc + d
        squares = part if squares is None else squares + part
        for i in range(2):
            src = pl.multiple_of((n * i + t) * chunk, chunk)
            dst = pl.multiple_of((2 * owner + i) * chunk, chunk)
            cur[:, pl.ds(dst, chunk)] = x[HALO_STEP:, pl.ds(src, chunk)]
    inverse = lax.rsqrt(squares / (n * width) + EPS)
    row0 = lax.axis_index("sp") * tok - halo
    mixed[...] = mix(acc * inverse, row0, wp[...], scale[...])
    first_sq[...] = to_rows([squares[HALO_STEP:]])


def to_rows(columns):
    rows = columns[0].shape[0]
    lane = lax.broadcasted_iota(jnp.int32, (rows, 128), 1)
    x = jnp.zeros((rows, 128), F32)
    for i, c in enumerate(columns):
        x = jnp.where(lane == i, c, x)
    eye = (lax.broadcasted_iota(jnp.int32, (8, 128), 0) == lax.broadcasted_iota(jnp.int32, (8, 128), 1)).astype(F32)
    return lax.dot_general(
        eye, x, (((1,), (1,)), ((), ())), precision=lax.Precision.HIGHEST, preferred_element_type=F32
    )


def to_columns(x):
    return jnp.transpose(x, (1, 0))


def branch_kernel(m0, m1, m2, m3, w_out, cur, gain, scaled, sums):
    t = lax.axis_index("tp")
    n = lax.axis_size("tp")
    acc = None
    for k, m in enumerate((m0, m1, m2, m3)):
        owner = lax.rem(t - k + n, n)
        w = w_out[:, owner].reshape(-1, w_out.shape[-1])
        d = dot_nt(m[...], w)
        acc = d if acc is None else acc + d
    out = acc * gain[...]
    scaled[...] = out
    sums[...] = to_rows([
        jnp.sum(acc * acc, axis=1, keepdims=True),
        jnp.sum(cur[...].astype(F32) * out, axis=1, keepdims=True),
        jnp.sum(out * out, axis=1, keepdims=True),
    ])


def new_scalars(part, other, before, width):
    total = part[...] + other[...]
    inv = lax.rsqrt(total[0:1] / width + EPS)
    squares = before[0:1] + 2.0 * inv * total[1:2] + inv * inv * total[2:3]
    return inv, jnp.maximum(squares, 0.0)


def project_kernel(width, part, other, before, cur, scaled, gain, w_in, p0, p1, p2, p3, new, after):
    t = lax.axis_index("tp")
    n = lax.axis_size("tp")
    inv, squares = new_scalars(part, other, before, width)
    after[...] = jnp.broadcast_to(squares, after.shape)
    column = to_columns(jnp.broadcast_to(inv, after.shape))[:, 0:1]
    value = (cur[...].astype(F32) + column * scaled[...]).astype(BF16)
    new[...] = value[HALO_STEP:]
    x = (value.astype(F32) * gain[...]).astype(BF16)
    for k, p in enumerate((p0, p1, p2, p3)):
        to = lax.rem(t + k, n)
        w = w_in[:, to].reshape(-1, w_in.shape[-1])
        p[...] = dot(x, w).astype(BF16)


def mix_kernel(halo, width, p0, p1, p2, p3, squares, wp, scale, mixed):
    rows = p0.shape[0]
    tok = rows - halo
    total = p0[...].astype(F32) + p1[...].astype(F32) + p2[...].astype(F32) + p3[...].astype(F32)
    inv = to_columns(lax.rsqrt(squares[...] / width + EPS))[:, 0:1]
    row0 = lax.axis_index("sp") * tok - halo
    mixed[...] = mix(total * inv, row0, wp[...], scale[...])


def tail_kernel(width, part, other, before, cur, scaled, p0, p1, p2, p3):
    t = lax.axis_index("tp")
    n = lax.axis_size("tp")
    inv, _ = new_scalars(part, other, before, width)
    column = to_columns(jnp.broadcast_to(inv, (8, inv.shape[1])))[:, 0:1]
    piece = p0.shape[1]
    for k, p in enumerate((p0, p1, p2, p3)):
        at = pl.ds(pl.multiple_of(lax.rem(t + k, n) * piece, piece), piece)
        p[...] = (cur[:, at].astype(F32) + column * scaled[:, at]).astype(BF16)


def place_kernel(r0, r1, r2, r3, out):
    t = lax.axis_index("tp")
    n = lax.axis_size("tp")
    chunk = r0.shape[1] // 2
    for k, r in enumerate((r0, r1, r2, r3)):
        owner = lax.rem(t - k + n, n)
        for i in range(2):
            at = pl.multiple_of((n * i + owner) * chunk, chunk)
            out[:, pl.ds(at, chunk)] = r[:, i * chunk : (i + 1) * chunk]


def per_device(stream, gain_pre, w_in, w_pool, pool_scale, w_out, gain_post):
    layers, width = gain_pre.shape
    tok, block = stream.shape
    n = lax.axis_size("tp")
    group = w_pool.shape[2]
    halo = layers * HALO_STEP
    t = lax.axis_index("tp")
    chunk = w_in.shape[1]
    per_col = lax.axis_size("sp") // n

    out_t = jnp.swapaxes(w_out, 1, 2)
    mine = lambda g: lax.dynamic_index_in_dim(
        g.reshape(layers, per_col, n, chunk), t, 2, keepdims=False
    ).reshape(layers, 1, block)
    pre_mine, post_mine = mine(gain_pre), mine(gain_post)
    scale = pool_scale.reshape(layers, 1, group)

    w_in0 = gathered(w_in[0:1])[0]
    shuffled0 = transposed_blocks(out_t[0:1])
    shuffled = [transposed_blocks(jnp.stack([w_in[l], out_t[l]])) for l in range(1, layers)]
    rim = from_behind(stream[tok - halo :])
    rows = jnp.concatenate([rim, stream], axis=0)
    others = shifts([(k, rows) for k in range(1, n)])
    w_out_l = gathered(shuffled0)[0]

    size = tok + halo
    mixed, cur, squares = vmem_call(
        functools.partial(head_kernel, halo),
        [
            shape((size - HALO_STEP, group), BF16),
            shape((size - HALO_STEP, block), BF16),
            shape((8, size - HALO_STEP), F32),
        ],
        rows,
        *others,
        gain_pre[0].reshape(n, 1, block),
        w_in0.reshape(n, block, group),
        w_pool[0, 0],
        scale[0],
        flops=2 * size * width * group,
        name="head",
    )
    for l in range(layers):
        size = mixed.shape[0]
        mixes = [mixed] + shifts([(k, mixed) for k in range(1, n)])
        scaled, part = vmem_call(
            branch_kernel,
            [shape((size, block), F32), shape((8, size), F32)],
            *mixes,
            w_out_l.reshape(per_col, n, chunk, group),
            cur,
            post_mine[l],
            flops=2 * size * n * group * block,
            name="branch",
        )
        part = part + pairwise(part, 0)
        other = pairwise(part, 1)
        if l == layers - 1:
            break
        w_in_l, w_out_l = gathered(shuffled[l])
        *parts, cur, squares = vmem_call(
            functools.partial(project_kernel, width),
            [shape((size, group), BF16)] * n + [shape((size - HALO_STEP, block), BF16), shape((8, size), F32)],
            part,
            other,
            squares,
            cur,
            scaled,
            pre_mine[l + 1],
            w_in_l.reshape(per_col, n, chunk, group),
            flops=2 * size * n * group * block,
            name="project",
        )
        received = shifts([(k, parts[k]) for k in range(1, n)])
        mixed = vmem_call(
            functools.partial(mix_kernel, size - tok, width),
            shape((size - HALO_STEP, group), BF16),
            parts[0],
            *received,
            squares,
            w_pool[l + 1, 0],
            scale[l + 1],
            flops=2 * size * group * group,
            name="mix",
        )
        squares = squares[:, HALO_STEP:]
    pieces = vmem_call(
        functools.partial(tail_kernel, width),
        [shape((tok, block // n), BF16)] * n,
        part,
        other,
        squares,
        cur,
        scaled,
        name="tail",
    )
    received = [pieces[0]] + shifts([(k, pieces[k]) for k in range(1, n)])
    return vmem_call(place_kernel, shape((tok, block), BF16), *received, name="place")


def solution(mesh):
    return jax.shard_map(
        per_device,
        mesh=mesh,
        in_specs=(
            P(("grp", "sp"), "tp"),
            P(),
            P(None, "sp", "tp"),
            P(None, "tp", None, None),
            P(None, "tp"),
            P(None, "tp", "sp"),
            P(),
        ),
        out_specs=P(("grp", "sp"), "tp"),
        check_vma=False,
    )
```
